256 devices in a mesh: ep: 32 (over z, x), tp: 8 (over y, core).
Axes of the slice: x: 4, y: 4, z: 8, core: 2. Of those that a mesh axis runs over, the one named last changes fastest.
Arguments:
- stream: bfloat16 [8192, 3072], P('ep'), may hold values from -30 to 30
- ffn_gain: bfloat16 [3072], replicated, may hold values from 0.099609375 to 1.8984375
- chosen: int32 [32, 1024], replicated, may hold values from 0 to 8191, as said below
- affinity: float32 [32, 1024], P('ep'), may hold values from 0.5 to 2
- w_gate: bfloat16 [32, 3072, 3072], P('ep', None, 'tp'), may hold values from -0.109375 to 0.109375
- w_up: bfloat16 [32, 3072, 3072], P('ep', None, 'tp'), may hold values from -0.109375 to 0.109375
- w_down: bfloat16 [32, 3072, 3072], P('ep', 'tp'), may hold values from -0.109375 to 0.109375
- final_gain: bfloat16 [3072], P('tp'), may hold values from 0.099609375 to 1.8984375
Outputs:
- normed: bfloat16 [8192, 3072], P('ep', 'tp')
The draws below stay inside these ranges and needn't reach their ends.
Inputs may be any that keep to these rules, and one draw needn't show every extreme that they name: `chosen`: row e holds 1024 distinct token numbers in ascending order. Of the 256 tokens of one index of ep, each expert reads at least one and at most 48; in every draw some expert reads exactly 48 from some index.
All inputs are finite; a program needn't handle non-finite values.
Results may differ from the reference program's by a relative error of at most 0.015.
Values may be sent and summed in bfloat16 or wider, within the bound.
No kernel may reach another device: no remote copies, remote signals or barrier semaphores. Data moves between devices by JAX's collectives and lax.ppermute only.
A program may use at most 128 MiB of HBM per device.

```python
import math
import jax
import jax.numpy as jnp
from jax import lax

D = 3072
FF = 3072
TOK_DEV = 256
TOKENS = 8192
EXPERTS = 32
CAP = 1024
N_EP = 32
N_TP = 8


def draw_stream(key, part):
    key_base, key_rows, key_cols = jax.random.split(key, 3)
    ramp = jnp.arange(D, dtype=jnp.float32) / D
    columns = jnp.exp(math.log(0.6) + ramp * math.log(3.0)) * jnp.exp(jax.random.uniform(key_cols, (D,), jnp.float32, -0.3, 0.3))
    base = jnp.clip(jax.random.normal(key_base, (TOKENS, D), jnp.float32), -4.0, 4.0)
    rows_scale = jnp.exp(jax.random.uniform(key_rows, (TOKENS, 1), jnp.float32, math.log(0.3), math.log(3.0)))
    return (base * rows_scale * columns[None, :]).astype(jnp.bfloat16)


def draw_chosen(key, part):
    mean_count = TOK_DEV // 8
    spread = TOK_DEV // 16
    pairs = N_EP // 2
    key_diff, key_pick, key_sign, key_score = jax.random.split(key, 4)
    diff = jax.random.randint(key_diff, (EXPERTS, pairs), -spread, spread + 1)
    forced = jax.random.randint(key_pick, (EXPERTS,), 0, pairs)
    signs = jax.random.randint(key_sign, (EXPERTS,), 0, 2) * 2 - 1
    diff = jnp.where(jnp.arange(pairs)[None, :] == forced[:, None], signs[:, None] * spread, diff)
    counts = jnp.stack([mean_count + diff, mean_count - diff], axis=2).reshape(EXPERTS, N_EP)
    scores = jax.random.randint(key_score, (EXPERTS, N_EP, TOK_DEV), 0, 65536) * TOK_DEV + jnp.arange(TOK_DEV)[None, None, :]
    ranks = jnp.argsort(jnp.argsort(scores, axis=-1), axis=-1)
    selected = (ranks < counts[:, :, None]).reshape(EXPERTS, TOKENS)
    positions = jnp.arange(TOKENS, dtype=jnp.int32)[None, :]
    keyed = jnp.where(selected, positions, positions + TOKENS)
    return jnp.sort(keyed, axis=-1)[:, :CAP].astype(jnp.int32)


def block_scale(own_key, shape, cuts, smallest, high):
    gain = 1.0
    for position, shards_of in cuts:
        steps = jax.random.uniform(jax.random.fold_in(jax.random.fold_in(own_key, 6), position), (shards_of,), jnp.float32, smallest / len(cuts), high / len(cuts))
        gain = gain * jnp.repeat(jnp.exp(steps), shape[position] // shards_of).reshape((-1,) + (1,) * (len(shape) - 1 - position))
    return gain


def centred(own_key, dims, scale, bound, shards=(), kind=jnp.bfloat16):
    values = jax.random.normal(own_key, dims, jnp.float32) * scale
    if len(shards) > 0:
        values = block_scale(own_key, dims, shards, -0.22, 0.18) * values
    return jnp.clip(values, min=-bound, max=bound).astype(kind)


def setup_inputs(seed: int = 0) -> dict:
    key_of = jax.random.split(jax.random.key(seed), 9)
    stream = draw_stream(jax.random.fold_in(key_of[8], 71), 0)
    ffn_gain = jnp.clip(1.0 + 0.18 * jax.random.normal(key_of[1], (D,), jnp.float32), 0.099609375, 1.8984375).astype(jnp.bfloat16)
    chosen = draw_chosen(jax.random.fold_in(key_of[8], 71), 0)
    affinity = jnp.clip(jnp.exp(math.log(2.0) - 1.3862944 * jax.random.uniform(key_of[3], (EXPERTS, CAP), jnp.float32) ** block_scale(key_of[3], (EXPERTS, CAP), ((0, 32),), -0.2, 0.2)), 0.5, 2.0)
    w_gate = centred(key_of[4], (EXPERTS, D, FF), D ** -0.5, 0.109375, ((0, 32), (2, 8)))
    w_up = centred(key_of[5], (EXPERTS, D, FF), D ** -0.5, 0.109375, ((0, 32), (2, 8)))
    w_down = centred(key_of[6], (EXPERTS, FF, D), FF ** -0.5, 0.109375, ((0, 32), (1, 8)))
    final_gain = jnp.clip(1.0 + 0.18 * jax.random.normal(key_of[7], (D,), jnp.float32), 0.099609375, 1.8984375).astype(jnp.bfloat16)
    return dict(stream=stream, ffn_gain=ffn_gain, chosen=chosen, affinity=affinity, w_gate=w_gate, w_up=w_up, w_down=w_down, final_gain=final_gain)


EPSILON = 1e-06

def reference(stream, ffn_gain, chosen, affinity, w_gate, w_up, w_down, final_gain):
    widened = stream.astype(jnp.float32)
    scale_in = lax.rsqrt(lax.optimization_barrier(jnp.mean(widened * widened, axis=-1, keepdims=True)) + EPSILON)
    normed_in = (widened * scale_in * ffn_gain.astype(jnp.float32)).astype(jnp.bfloat16)
    block = FF // N_TP

    def one_expert(update, items):
        token_ids, weights, gate_rows, up_rows, down_rows = items
        picked = normed_in[token_ids]
        gate = jnp.dot(picked, gate_rows, preferred_element_type=jnp.float32)
        up = jnp.dot(picked, up_rows, preferred_element_type=jnp.float32)
        hidden = (jax.nn.silu(gate) * up).astype(jnp.bfloat16)
        blocks = hidden.reshape(CAP, N_TP, block).astype(jnp.float32)
        down_blocks = down_rows.reshape(N_TP, block, D).astype(jnp.float32)
        partial_value = jnp.einsum('cjf,jfd->jcd', blocks, down_blocks).astype(jnp.bfloat16)
        summed = lax.optimization_barrier(jnp.sum(partial_value.astype(jnp.float32), axis=0))
        result = (summed * weights[:, None]).astype(jnp.bfloat16)
        return (update.at[token_ids].add(result.astype(jnp.float32)), None)
    update, unused = lax.scan(one_expert, jnp.zeros((TOKENS, D), jnp.float32), (chosen, affinity, w_gate, w_up, w_down))
    merged = widened + update
    scale_out = lax.rsqrt(lax.optimization_barrier(jnp.mean(merged * merged, axis=-1, keepdims=True)) + EPSILON)
    return (merged * scale_out * final_gain.astype(jnp.float32)).astype(jnp.bfloat16)
```

```python
import functools

import jax
import jax.numpy as jnp
from jax import lax
from jax.experimental import pallas as pl
from jax.experimental.pallas import tpu as pltpu
from jax.sharding import PartitionSpec as P

EPSILON = 1e-06
LANES = 128
F32 = jnp.float32
BF16 = jnp.bfloat16


def exchanged(array, axis, mask):
    devices = lax.axis_size(axis)
    return lax.ppermute(array, axis, [(i, i ^ mask) for i in range(devices)])


def cost(flops, moved):
    return pl.CostEstimate(flops=int(flops), bytes_accessed=int(moved), transcendentals=0)


def shape_of(shape, dtype):
    return jax.ShapeDtypeStruct(shape, dtype)


def whole(shape):
    return pl.BlockSpec(shape, lambda *_: (0,) * len(shape))


def send_kernel(chunks, column_ref, stream_ref, own_ref, gain_ref, sel_ref, *out_refs):
    x = stream_ref[...].astype(F32)
    scale = lax.rsqrt(jnp.mean(x * x, axis=-1, keepdims=True) + EPSILON)
    own = (own_ref[...].astype(F32) * scale * gain_ref[...].astype(F32)).astype(BF16)
    tokens = own.shape[0]
    sel = sel_ref[...]
    hit = lax.broadcasted_iota(jnp.int32, (tokens, sel.shape[1]), 0) == sel
    placed = jnp.where(hit, 1.0, 0.0).astype(BF16)
    rows = lax.dot_general(
        placed, own, (((0,), (0,)), ((), ())), preferred_element_type=F32
    ).astype(BF16)
    for j in range(chunks):
        out_refs[j][...] = rows[:, j * LANES : (j + 1) * LANES]


def outgoing_rows(column, stream, gain, sel, share, chunks):
    tokens, width = stream.shape
    slots = sel.shape[1]
    return pl.pallas_call(
        functools.partial(send_kernel, chunks),
        grid_spec=pltpu.PrefetchScalarGridSpec(
            num_scalar_prefetch=1,
            grid=(1,),
            in_specs=[
                whole((tokens, width)),
                pl.BlockSpec((tokens, share), lambda i, col: (0, col[0])),
                pl.BlockSpec((1, share), lambda i, col: (0, col[0])),
                whole((1, slots)),
            ],
            out_specs=[whole((slots, LANES))] * chunks,
        ),
        out_shape=[shape_of((slots, LANES), BF16)] * chunks,
        cost_estimate=cost(2 * slots * tokens * share, 2 * tokens * width + 2 * slots * share),
        name="send_rows",
    )(column, stream, stream, gain, sel)


def compact_kernel(inv_ref, arrived_ref, out_ref):
    tile, slots = out_ref.shape[0], inv_ref.shape[1]
    at = lax.broadcasted_iota(jnp.int32, (tile, slots), 0) + pl.program_id(0) * tile
    hit = jnp.where(at == inv_ref[...], 1.0, 0.0).astype(BF16)
    out_ref[...] = jnp.dot(hit, arrived_ref[...], preferred_element_type=F32).astype(BF16)


def compacted(inv, arrived, picks):
    slots, width = arrived.shape
    tile = 256
    return pl.pallas_call(
        compact_kernel,
        grid=(picks // tile,),
        in_specs=[whole((1, slots)), whole((slots, width))],
        out_specs=pl.BlockSpec((tile, width), lambda i: (i, 0)),
        out_shape=shape_of((picks, width), BF16),
        cost_estimate=cost(2 * picks * slots * width, 2 * slots * width),
        name="compact_rows",
    )(inv, arrived)


ORDER = (0, 1, 2, 3, 6, 7)


def ffn_kernel(first, last, group_ref, *refs):
    pieces = refs[:6]
    halves = refs[6:10]
    gates = refs[10:18]
    ups = refs[18:26]
    rest = refs[26:]
    upper = pl.program_id(0) >= pl.num_programs(0) // 2
    far = [jnp.where(upper, halves[2 * k + 1][...], halves[2 * k][...]) for k in range(2)]
    by_mask = {mask: pieces[i][...] for i, mask in enumerate(ORDER)}
    by_mask[4], by_mask[5] = far
    units = gates[0].shape[1]
    total = None
    for pair in range(4):
        low, high = 2 * pair, 2 * pair + 1
        left = jnp.concatenate([by_mask[low], by_mask[high]], axis=1)
        weights = jnp.concatenate(
            [
                jnp.concatenate([gates[low][...], gates[high][...]], axis=0),
                jnp.concatenate([ups[low][...], ups[high][...]], axis=0),
            ],
            axis=1,
        )
        part = jnp.dot(left, weights, preferred_element_type=F32)
        total = part if total is None else total + part
    if not first:
        total = total + rest[0][...]
    out_ref = rest[-1]
    if last:
        gate, up = total[:, :units], total[:, units:]
        out_ref[...] = (gate / (1.0 + jnp.exp(-gate)) * up).astype(BF16)
    else:
        out_ref[...] = total


def ffn_chunk(group, pieces, halves, w_gate, w_up, acc, chunk, chunks, last):
    picks = pieces[0].shape[0]
    units = w_gate.shape[1]
    tile = 256
    steps = picks // tile
    first = acc is None
    row_spec = pl.BlockSpec((tile, LANES), lambda i, g: (i, 0))
    low_spec = pl.BlockSpec((tile, LANES), lambda i, g: (jnp.minimum(i, steps // 2 - 1), 0))
    high_spec = pl.BlockSpec((tile, LANES), lambda i, g: (jnp.maximum(i - steps // 2, 0), 0))

    def weight_spec(mask):
        return pl.BlockSpec((LANES, units), lambda i, g: ((g[0] ^ mask) * chunks + chunk, 0))

    weight_specs = [weight_spec(mask) for mask in range(8)]
    acc_spec = pl.BlockSpec((tile, 2 * units), lambda i, g: (i, 0))
    out_width, out_type = (units, BF16) if last else (2 * units, F32)
    return pl.pallas_call(
        functools.partial(ffn_kernel, first, last),
        grid_spec=pltpu.PrefetchScalarGridSpec(
            num_scalar_prefetch=1,
            grid=(steps,),
            in_specs=[row_spec] * 6
            + [low_spec, high_spec] * 2
            + weight_specs * 2
            + ([] if first else [acc_spec]),
            out_specs=pl.BlockSpec((tile, out_width), lambda i, g: (i, 0)),
        ),
        out_shape=shape_of((picks, out_width), out_type),
        input_output_aliases={} if first or last else {27: 0},
        cost_estimate=cost(2 * picks * 8 * LANES * 2 * units, 12 * picks * units),
        name="gate_up",
    )(group, *pieces, *halves, *([w_gate] * 8), *([w_up] * 8), *([] if first else [acc]))


def down_kernel(group_ref, hidden_ref, *refs):
    weights, (keep_ref, give_ref) = refs[:8], refs[8:]
    hidden = hidden_ref[...]
    for k, out_ref in enumerate((keep_ref, give_ref)):
        side = jnp.concatenate([weights[2 * d + k][...] for d in range(4)], axis=1)
        out_ref[...] = jnp.dot(hidden, side, preferred_element_type=F32).astype(BF16)


def down_chunk(group, hidden, w_down, chunk, chunks):
    picks, units = hidden.shape
    tile = 256

    def weight_spec(mask):
        return pl.BlockSpec((units, LANES), lambda i, g: (0, (g[0] ^ mask) * chunks + chunk))

    row_spec = pl.BlockSpec((tile, 4 * LANES), lambda i, g: (i, 0))
    return pl.pallas_call(
        down_kernel,
        grid_spec=pltpu.PrefetchScalarGridSpec(
            num_scalar_prefetch=1,
            grid=(picks // tile,),
            in_specs=[pl.BlockSpec((tile, units), lambda i, g: (i, 0))]
            + [weight_spec(mask) for mask in range(8)],
            out_specs=[row_spec, row_spec],
        ),
        out_shape=[shape_of((picks, 4 * LANES), BF16)] * 2,
        cost_estimate=cost(2 * picks * 8 * LANES * units, 16 * picks * LANES),
        name="down",
    )(group, hidden, *([w_down] * 8))


def pair_kernel(keep_ref, came_ref, a_keep, a_send, b_keep, b_send):
    total = (keep_ref[...].astype(F32) + came_ref[...].astype(F32)).astype(BF16)
    half = total.shape[0] // 2
    block = [total[:, d * LANES : (d + 1) * LANES] for d in range(4)]
    for ref, masks, low in (
        (a_keep, (0, 3), True),
        (a_send, (1, 2), True),
        (b_keep, (0, 1), False),
        (b_send, (3, 2), False),
    ):
        for n, d in enumerate(masks):
            rows = block[d][:half] if low else block[d][half:]
            ref[:, n * LANES : (n + 1) * LANES] = rows


def pair_sums(keep, came):
    picks = keep.shape[0]
    half = (picks // 2, 2 * LANES)
    return pl.pallas_call(
        pair_kernel,
        out_shape=[shape_of(half, BF16)] * 4,
        cost_estimate=cost(picks * 4 * LANES, 3 * picks * 4 * LANES * 2),
        name="pair_sums",
    )(keep, came)


def quad_kernel(a_keep, a_came, b_keep, b_came, a_own, a_next, b_own, b_next):
    for keep, came, own, following in (
        (a_keep, a_came, a_own, a_next),
        (b_keep, b_came, b_own, b_next),
    ):
        total = keep[...].astype(F32) + came[...].astype(F32)
        own[...] = total[:, :LANES]
        following[...] = total[:, LANES:].astype(BF16)


def quad_sums(a_keep, a_came, b_keep, b_came):
    half = a_keep.shape[0]
    kinds = [shape_of((half, LANES), F32), shape_of((half, LANES), BF16)]
    return pl.pallas_call(
        quad_kernel,
        out_shape=kinds * 2,
        cost_estimate=cost(half * 4 * LANES, half * LANES * 20),
        name="quad_sums",
    )(a_keep, a_came, b_keep, b_came)


def leave_kernel(a_own, a_came, b_own, b_came, weight_ref, arrival_ref, out_ref, rows_ref):
    half = a_own.shape[0]

    @pl.when(pl.program_id(0) == 0)
    def _():
        weight = weight_ref[...]
        top = (a_own[...] + a_came[...].astype(F32)) * weight[:half]
        low = (b_own[...] + b_came[...].astype(F32)) * weight[half:]
        rows_ref[:half] = top.astype(BF16)
        rows_ref[half:] = low.astype(BF16)

    tile, picks = out_ref.shape[0], arrival_ref.shape[1]
    at = lax.broadcasted_iota(jnp.int32, (tile, picks), 0) + pl.program_id(0) * tile
    hit = jnp.where(at == arrival_ref[...], 1.0, 0.0).astype(BF16)
    out_ref[...] = jnp.dot(hit, rows_ref[...], preferred_element_type=F32).astype(BF16)


def leaving_rows(a_own, a_came, b_own, b_came, weight, arrival, slots):
    half = a_own.shape[0]
    tile = 256
    return pl.pallas_call(
        leave_kernel,
        grid=(slots // tile,),
        in_specs=[whole((half, LANES))] * 4 + [whole((2 * half, 1)), whole((1, 2 * half))],
        out_specs=pl.BlockSpec((tile, LANES), lambda i: (i, 0)),
        out_shape=shape_of((slots, LANES), BF16),
        scratch_shapes=[pltpu.VMEM((2 * half, LANES), BF16)],
        cost_estimate=cost(4 * slots * half * LANES, 2 * slots * LANES),
        name="leave_rows",
    )(a_own, a_came, b_own, b_came, weight, arrival)


def merge_kernel(chunks, column_ref, own_ref, sel_ref, *refs):
    returned, (merged_ref, square_ref) = refs[:chunks], refs[chunks:]
    tokens = own_ref.shape[0]
    sel = sel_ref[...]
    hit = lax.broadcasted_iota(jnp.int32, (tokens, sel.shape[1]), 0) == sel
    placed = jnp.where(hit, 1.0, 0.0).astype(BF16)
    came = jnp.concatenate([ref[...] for ref in returned], axis=1)
    merged = own_ref[...].astype(F32) + jnp.dot(placed, came, preferred_element_type=F32)
    merged_ref[...] = merged
    square_ref[...] = jnp.sum(merged * merged, axis=1, keepdims=True)


def merged_rows(column, stream, sel, returned, share):
    tokens = stream.shape[0]
    slots = sel.shape[1]
    chunks = len(returned)
    return pl.pallas_call(
        functools.partial(merge_kernel, chunks),
        grid_spec=pltpu.PrefetchScalarGridSpec(
            num_scalar_prefetch=1,
            grid=(1,),
            in_specs=[
                pl.BlockSpec((tokens, share), lambda i, col: (0, col[0])),
                whole((1, slots)),
            ]
            + [whole((slots, LANES))] * chunks,
            out_specs=[whole((tokens, share)), whole((tokens, 1))],
        ),
        out_shape=[shape_of((tokens, share), F32), shape_of((tokens, 1), F32)],
        cost_estimate=cost(2 * slots * tokens * share, 2 * slots * share),
        name="merge_rows",
    )(column, stream, sel, *returned)


def on_device(stream, ffn_gain, chosen, affinity, w_gate, w_up, w_down, final_gain):
    tok_rows, model_width = stream.shape
    experts, picks = chosen.shape
    ep_count = lax.axis_size("ep")
    tp_count = lax.axis_size("tp")
    device = lax.axis_index("ep")
    column = lax.axis_index("tp").astype(jnp.int32)
    share = model_width // tp_count
    chunks = share // LANES
    slots = 3 * tok_rows // 16
    group = column.reshape(1)

    base = device * tok_rows
    begin = jnp.sum((chosen < base).astype(jnp.int32), axis=1)
    end = jnp.sum((chosen < base + tok_rows).astype(jnp.int32), axis=1)
    slot_range = jnp.arange(slots, dtype=jnp.int32)
    places = jnp.arange(picks, dtype=jnp.int32)
    want = begin[:, None] + slot_range[None, :]
    found = jnp.sum(
        jnp.where(places[None, None, :] == want[:, :, None], chosen[:, None, :], 0), axis=2
    )
    sel = jnp.where(want < end[:, None], found - base, -1).reshape(1, experts * slots)

    row = lax.dynamic_index_in_dim(chosen, device, 0, keepdims=True)
    edges = jnp.arange(ep_count, dtype=jnp.int32)[:, None] * tok_rows
    starts = jnp.sum((row < edges).astype(jnp.int32), axis=1)
    stops = jnp.sum((row < edges + tok_rows).astype(jnp.int32), axis=1)
    row_want = starts[:, None] + slot_range[None, :]
    inv = jnp.where(row_want < stops[:, None], row_want, -1).reshape(1, ep_count * slots)
    mine = (row >= edges) & (row < edges + tok_rows)
    arrival = jnp.sum(
        jnp.where(
            mine,
            jnp.arange(ep_count, dtype=jnp.int32)[:, None] * slots
            + places[None, :]
            - starts[:, None],
            0,
        ),
        axis=0,
        keepdims=True,
    )
    weight = affinity.reshape(picks, 1)

    half = picks // 2
    gate_rows, up_rows, down_rows = w_gate[0], w_up[0], w_down[0]
    outgoing = outgoing_rows(group, stream, ffn_gain.reshape(1, -1), sel, share, chunks)
    hidden = None
    for j in range(chunks):
        arrived = lax.all_to_all(
            outgoing[j].reshape(experts, slots, LANES), "ep", split_axis=0, concat_axis=0, tiled=True
        )
        own = compacted(inv, arrived.reshape(-1, LANES), picks)
        near = exchanged(own, "tp", 2)
        back = exchanged(own, "tp", 6)
        far_low = exchanged(near[:half], "tp", 6)
        far_high = exchanged(back[half:], "tp", 2)
        pieces = []
        for piece in (own, near, back):
            pieces += [piece, exchanged(piece, "tp", 1)]
        halves = [far_low, far_high, exchanged(far_low, "tp", 1), exchanged(far_high, "tp", 1)]
        hidden = ffn_chunk(
            group, pieces, halves, gate_rows, up_rows, hidden, j, chunks, j == chunks - 1
        )
    returned = []
    for j in range(chunks):
        keep, give = down_chunk(group, hidden, down_rows, j, chunks)
        a_keep, a_send, b_keep, b_send = pair_sums(keep, exchanged(give, "tp", 1))
        a_own, a_next, b_own, b_next = quad_sums(
            a_keep, exchanged(a_send, "tp", 2), b_keep, exchanged(b_send, "tp", 6)
        )
        leaving = leaving_rows(
            a_own,
            exchanged(a_next, "tp", 6),
            b_own,
            exchanged(b_next, "tp", 2),
            weight,
            arrival,
            ep_count * slots,
        )
        came = lax.all_to_all(
            leaving.reshape(ep_count, slots, LANES), "ep", split_axis=0, concat_axis=0, tiled=True
        )
        returned.append(came.reshape(-1, LANES))
    merged, squares = merged_rows(group, stream, sel, returned, share)
    totals = squares.reshape(1, tok_rows)
    for mask in (1, 2, 6):
        totals = totals + exchanged(totals, "tp", mask)
    scale_out = lax.rsqrt(totals.reshape(tok_rows, 1) / model_width + EPSILON)
    return (merged * scale_out * final_gain.astype(F32)[None, :]).astype(BF16)


def solution(mesh):
    return jax.shard_map(
        on_device,
        mesh=mesh,
        in_specs=(
            P("ep", None),
            P(),
            P(),
            P("ep", None),
            P("ep", None, "tp"),
            P("ep", None, "tp"),
            P("ep", "tp", None),
            P("tp"),
        ),
        out_specs=P("ep", "tp"),
        check_vma=False,
    )
```

```python
import functools

import jax
import jax.numpy as jnp
from jax import lax
from jax.experimental import pallas as pl
from jax.experimental.pallas import tpu as pltpu
from jax.sharding import PartitionSpec as P

EPSILON = 1e-06
F32 = jnp.float32
BF16 = jnp.bfloat16


def exchanged(array, axis, mask):
    devices = lax.axis_size(axis)
    return lax.ppermute(array, axis, [(i, i ^ mask) for i in range(devices)])


def cost(flops, moved):
    return pl.CostEstimate(flops=int(flops), bytes_accessed=int(moved), transcendentals=0)


PARAMS = pltpu.CompilerParams(vmem_limit_bytes=28 * 1024 * 1024)


def shape_of(shape, dtype):
    return jax.ShapeDtypeStruct(shape, dtype)


def whole(shape):
    return pl.BlockSpec(shape, lambda *_: (0,) * len(shape))


def send_kernel(column_ref, stream_ref, own_ref, gain_ref, sel_ref, out_ref):
    x = stream_ref[...].astype(F32)
    scale = lax.rsqrt(jnp.mean(x * x, axis=-1, keepdims=True) + EPSILON)
    own = (own_ref[...].astype(F32) * scale * gain_ref[...].astype(F32)).astype(BF16)
    tokens = own.shape[0]
    sel = sel_ref[...]
    hit = lax.broadcasted_iota(jnp.int32, (tokens, sel.shape[1]), 0) == sel
    placed = jnp.where(hit, 1.0, 0.0).astype(BF16)
    out_ref[...] = lax.dot_general(
        placed, own, (((0,), (0,)), ((), ())), preferred_element_type=F32
    ).astype(BF16)


def outgoing_rows(column, stream, gain, sel, share):
    tokens, width = stream.shape
    slots = sel.shape[1]
    return pl.pallas_call(
        send_kernel,
        grid_spec=pltpu.PrefetchScalarGridSpec(
            num_scalar_prefetch=1,
            grid=(1,),
            in_specs=[
                whole((tokens, width)),
                pl.BlockSpec((tokens, share), lambda i, col: (0, col[0])),
                pl.BlockSpec((1, share), lambda i, col: (0, col[0])),
                whole((1, slots)),
            ],
            out_specs=whole((slots, share)),
        ),
        out_shape=shape_of((slots, share), BF16),
        cost_estimate=cost(2 * slots * tokens * share, 2 * tokens * width + 2 * slots * share),
        compiler_params=PARAMS,
        name="send_rows",
    )(column, stream, stream, gain, sel)


def compact_kernel(inv_ref, arrived_ref, out_ref):
    tile, slots = out_ref.shape[0], inv_ref.shape[1]
    at = lax.broadcasted_iota(jnp.int32, (tile, slots), 0) + pl.program_id(0) * tile
    hit = jnp.where(at == inv_ref[...], 1.0, 0.0).astype(BF16)
    out_ref[...] = jnp.dot(hit, arrived_ref[...], preferred_element_type=F32).astype(BF16)


def compacted(inv, arrived, picks):
    slots, width = arrived.shape
    tile = picks // 2
    return pl.pallas_call(
        compact_kernel,
        grid=(picks // tile,),
        in_specs=[whole((1, slots)), whole((slots, width))],
        out_specs=pl.BlockSpec((tile, width), lambda i: (i, 0)),
        out_shape=shape_of((picks, width), BF16),
        cost_estimate=cost(2 * picks * slots * width, 2 * slots * width),
        compiler_params=PARAMS,
        name="compact_rows",
    )(inv, arrived)


EARLY = (0, 1, 2, 3, 6, 7)


def products(pieces, gates, ups):
    total = None
    for piece, gate, up in zip(pieces, gates, ups):
        weights = jnp.concatenate([gate[...], up[...]], axis=1)
        part = jnp.dot(piece, weights, preferred_element_type=F32)
        total = part if total is None else total + part
    return total


def early_kernel(group_ref, *refs):
    n = len(EARLY)
    pieces = [ref[...] for ref in refs[:n]]
    refs[-1][...] = products(pieces, refs[n : 2 * n], refs[2 * n : 3 * n])


def late_kernel(group_ref, low, high, low_x, high_x, g4, g5, u4, u5, acc_ref, out_ref):
    upper = pl.program_id(0) >= pl.num_programs(0) // 2
    pieces = [
        jnp.where(upper, high[...], low[...]),
        jnp.where(upper, high_x[...], low_x[...]),
    ]
    total = acc_ref[...] + products(pieces, (g4, g5), (u4, u5))
    units = out_ref.shape[1]
    gate, up = total[:, :units], total[:, units:]
    out_ref[...] = (gate / (1.0 + jnp.exp(-gate)) * up).astype(BF16)


def weight_specs(masks, share, units):
    def spec(mask):
        return pl.BlockSpec((share, units), lambda i, g: (g[0] ^ mask, 0))

    return [spec(mask) for mask in masks]


def early_products(group, pieces, w_gate, w_up):
    picks, share = pieces[0].shape
    units = w_gate.shape[1]
    tile = 256
    n = len(EARLY)
    return pl.pallas_call(
        early_kernel,
        grid_spec=pltpu.PrefetchScalarGridSpec(
            num_scalar_prefetch=1,
            grid=(picks // tile,),
            in_specs=[pl.BlockSpec((tile, share), lambda i, g: (i, 0))] * n
            + weight_specs(EARLY, share, units) * 2,
            out_specs=pl.BlockSpec((tile, 2 * units), lambda i, g: (i, 0)),
        ),
        out_shape=shape_of((picks, 2 * units), F32),
        cost_estimate=cost(4 * picks * n * share * units, 2 * n * share * (picks + 2 * units)),
        compiler_params=PARAMS,
        name="gate_up_early",
    )(group, *pieces, *([w_gate] * n), *([w_up] * n))


def late_products(group, halves, w_gate, w_up, acc):
    half, share = halves[0].shape
    picks = 2 * half
    units = w_gate.shape[1]
    tile = 256
    steps = picks // tile
    low_spec = pl.BlockSpec((tile, share), lambda i, g: (jnp.minimum(i, steps // 2 - 1), 0))
    high_spec = pl.BlockSpec((tile, share), lambda i, g: (jnp.maximum(i - steps // 2, 0), 0))
    return pl.pallas_call(
        late_kernel,
        grid_spec=pltpu.PrefetchScalarGridSpec(
            num_scalar_prefetch=1,
            grid=(steps,),
            in_specs=[low_spec, high_spec] * 2
            + weight_specs((4, 5), share, units) * 2
            + [pl.BlockSpec((tile, 2 * units), lambda i, g: (i, 0))],
            out_specs=pl.BlockSpec((tile, units), lambda i, g: (i, 0)),
        ),
        out_shape=shape_of((picks, units), BF16),
        cost_estimate=cost(8 * picks * share * units, 4 * share * (picks + 2 * units)),
        compiler_params=PARAMS,
        name="gate_up_late",
    )(group, *halves, *([w_gate] * 2), *([w_up] * 2), acc)


def down_kernel(group_ref, hidden_ref, *refs):
    weights, out_ref = refs[:4], refs[4]
    side = jnp.concatenate([ref[...] for ref in weights], axis=1)
    out_ref[...] = jnp.dot(hidden_ref[...], side, preferred_element_type=F32).astype(BF16)


def down_products(group, hidden, w_down, core):
    picks, units = hidden.shape
    share = w_down.shape[1] // 8
    tile = 256

    def spec(mask):
        return pl.BlockSpec((units, share), lambda i, g: (0, g[0] ^ mask))

    return pl.pallas_call(
        down_kernel,
        grid_spec=pltpu.PrefetchScalarGridSpec(
            num_scalar_prefetch=1,
            grid=(picks // tile,),
            in_specs=[pl.BlockSpec((tile, units), lambda i, g: (i, 0))]
            + [spec(2 * d + core) for d in range(4)],
            out_specs=pl.BlockSpec((tile, 4 * share), lambda i, g: (i, 0)),
        ),
        out_shape=shape_of((picks, 4 * share), BF16),
        cost_estimate=cost(8 * picks * share * units, 8 * (picks + units) * share),
        compiler_params=PARAMS,
        name="down",
    )(group, hidden, *([w_down] * 4))


def added(*refs):
    total = refs[0][...].astype(F32)
    for ref in refs[1:]:
        total = total + ref[...].astype(F32)
    return total


def pair_kernel(*refs):
    (a_ref, b_ref) = refs[8:]
    share = refs[0].shape[1]
    for out_ref, first in ((a_ref, 0), (b_ref, 4)):
        for n in range(2):
            out_ref[:, n * share : (n + 1) * share] = added(
                refs[first + 2 * n], refs[first + 2 * n + 1]
            ).astype(BF16)


def pair_sums(keep, came, share):
    picks = keep.shape[0]
    half = picks // 2
    tile = half // 2

    def spec(side, d):
        return pl.BlockSpec((tile, share), lambda i: (i + side * (half // tile), d))

    picked = [(0, 1), (0, 2), (1, 3), (1, 2)]
    specs = []
    for side, d in picked:
        specs += [spec(side, d)] * 2
    return pl.pallas_call(
        pair_kernel,
        grid=(half // tile,),
        in_specs=specs,
        out_specs=[pl.BlockSpec((tile, 2 * share), lambda i: (i, 0))] * 2,
        out_shape=[shape_of((half, 2 * share), BF16)] * 2,
        cost_estimate=cost(half * 4 * share, 24 * half * share),
        compiler_params=PARAMS,
        name="pair_sums",
    )(*([keep, came] * 4))


def quad_kernel(a0, a1, a2, b0, b1, b2, a_ref, b_ref):
    a_ref[...] = added(a0, a1, a2).astype(BF16)
    b_ref[...] = added(b0, b1, b2).astype(BF16)


def quad_sums(keep, came, a_came, b_came, share):
    picks = keep.shape[0]
    half = picks // 2
    tile = half // 2

    def spec(side, d):
        return pl.BlockSpec((tile, share), lambda i: (i + side * (half // tile), d))

    second = pl.BlockSpec((tile, share), lambda i: (i, 1))
    out = pl.BlockSpec((tile, share), lambda i: (i, 0))
    return pl.pallas_call(
        quad_kernel,
        grid=(half // tile,),
        in_specs=[spec(0, 3), spec(0, 3), second, spec(1, 1), spec(1, 1), second],
        out_specs=[out, out],
        out_shape=[shape_of((half, share), BF16)] * 2,
        cost_estimate=cost(half * 4 * share, 16 * half * share),
        compiler_params=PARAMS,
        name="quad_sums",
    )(keep, came, a_came, keep, came, b_came)


def leave_kernel(keep, came, a1, b1, a2, b2, weight_ref, arrival_ref, out_ref, rows_ref):
    half = a1.shape[0]

    @pl.when(pl.program_id(0) == 0)
    def _():
        total = added(keep, came)
        weight = weight_ref[...]
        rows_ref[:half] = ((total[:half] + added(a1, a2)) * weight[:half]).astype(BF16)
        rows_ref[half:] = ((total[half:] + added(b1, b2)) * weight[half:]).astype(BF16)

    tile, picks = out_ref.shape[0], arrival_ref.shape[1]
    at = lax.broadcasted_iota(jnp.int32, (tile, picks), 0) + pl.program_id(0) * tile
    hit = jnp.where(at == arrival_ref[...], 1.0, 0.0).astype(BF16)
    out_ref[...] = jnp.dot(hit, rows_ref[...], preferred_element_type=F32).astype(BF16)


def leaving_rows(keep, came, a1, b1, a2, b2, weight, arrival, slots, share):
    picks = keep.shape[0]
    half = picks // 2
    tile = slots // 3
    return pl.pallas_call(
        leave_kernel,
        grid=(slots // tile,),
        in_specs=[whole((picks, share))] * 2
        + [whole((half, share))] * 4
        + [whole((picks, 1)), whole((1, picks))],
        out_specs=pl.BlockSpec((tile, share), lambda i: (i, 0)),
        out_shape=shape_of((slots, share), BF16),
        scratch_shapes=[pltpu.VMEM((picks, share), BF16)],
        cost_estimate=cost(2 * slots * picks * share, 2 * (slots + 4 * picks) * share),
        compiler_params=PARAMS,
        name="leave_rows",
    )(keep, came, a1, b1, a2, b2, weight, arrival)


def merge_kernel(column_ref, own_ref, sel_ref, came_ref, merged_ref, square_ref):
    tokens = own_ref.shape[0]
    sel = sel_ref[...]
    hit = lax.broadcasted_iota(jnp.int32, (tokens, sel.shape[1]), 0) == sel
    placed = jnp.where(hit, 1.0, 0.0).astype(BF16)
    update = jnp.dot(placed, came_ref[...], preferred_element_type=F32)
    merged = own_ref[...].astype(F32) + update
    merged_ref[...] = merged
    square_ref[...] = jnp.sum(merged * merged, axis=1, keepdims=True)


def merged_rows(column, stream, sel, came, share):
    tokens = stream.shape[0]
    slots = sel.shape[1]
    return pl.pallas_call(
        merge_kernel,
        grid_spec=pltpu.PrefetchScalarGridSpec(
            num_scalar_prefetch=1,
            grid=(1,),
            in_specs=[
                pl.BlockSpec((tokens, share), lambda i, col: (0, col[0])),
                whole((1, slots)),
                whole((slots, share)),
            ],
            out_specs=[whole((tokens, share)), whole((tokens, 1))],
        ),
        out_shape=[shape_of((tokens, share), F32), shape_of((tokens, 1), F32)],
        cost_estimate=cost(2 * slots * tokens * share, 2 * slots * share),
        compiler_params=PARAMS,
        name="merge_rows",
    )(column, stream, sel, came)


def on_device(stream, ffn_gain, chosen, affinity, w_gate, w_up, w_down, final_gain):
    tok_rows, model_width = stream.shape
    experts, picks = chosen.shape
    ep_count = lax.axis_size("ep")
    tp_count = lax.axis_size("tp")
    device = lax.axis_index("ep")
    column = lax.axis_index("tp").astype(jnp.int32)
    share = model_width // tp_count
    slots = 3 * tok_rows // 16
    group = column.reshape(1)

    base = device * tok_rows
    begin = jnp.sum((chosen < base).astype(jnp.int32), axis=1)
    end = jnp.sum((chosen < base + tok_rows).astype(jnp.int32), axis=1)
    slot_range = jnp.arange(slots, dtype=jnp.int32)
    places = jnp.arange(picks, dtype=jnp.int32)
    want = begin[:, None] + slot_range[None, :]
    found = jnp.sum(
        jnp.where(places[None, None, :] == want[:, :, None], chosen[:, None, :], 0), axis=2
    )
    sel = jnp.where(want < end[:, None], found - base, -1).reshape(1, experts * slots)

    row = lax.dynamic_index_in_dim(chosen, device, 0, keepdims=True)
    edges = jnp.arange(ep_count, dtype=jnp.int32)[:, None] * tok_rows
    starts = jnp.sum((row < edges).astype(jnp.int32), axis=1)
    stops = jnp.sum((row < edges + tok_rows).astype(jnp.int32), axis=1)
    row_want = starts[:, None] + slot_range[None, :]
    inv = jnp.where(row_want < stops[:, None], row_want, -1).reshape(1, ep_count * slots)
    mine = (row >= edges) & (row < edges + tok_rows)
    arrival = jnp.sum(
        jnp.where(
            mine,
            jnp.arange(ep_count, dtype=jnp.int32)[:, None] * slots
            + places[None, :]
            - starts[:, None],
            0,
        ),
        axis=0,
        keepdims=True,
    )
    weight = affinity.reshape(picks, 1)

    half = picks // 2
    gate_rows, up_rows, down_rows = w_gate[0], w_up[0], w_down[0]
    outgoing = outgoing_rows(group, stream, ffn_gain.reshape(1, -1), sel, share)
    arrived = lax.all_to_all(
        outgoing.reshape(experts, slots, share), "ep", split_axis=0, concat_axis=0, tiled=True
    )
    own = compacted(inv, arrived.reshape(-1, share), picks)
    near = exchanged(own, "tp", 2)
    back = exchanged(own, "tp", 6)
    far_low = exchanged(near[:half], "tp", 6)
    far_high = exchanged(back[half:], "tp", 2)
    pieces = []
    for piece in (own, near, back):
        pieces += [piece, exchanged(piece, "tp", 1)]
    acc = early_products(group, pieces, gate_rows, up_rows)
    far_low, far_high, acc = lax.optimization_barrier((far_low, far_high, acc))
    halves = [far_low, far_high, exchanged(far_low, "tp", 1), exchanged(far_high, "tp", 1)]
    hidden = late_products(group, halves, gate_rows, up_rows, acc)

    came = exchanged(down_products(group, hidden, down_rows, 1), "tp", 1)
    keep = down_products(group, hidden, down_rows, 0)
    a_send, b_send = pair_sums(keep, came, share)
    a1, b1 = exchanged(a_send, "tp", 2), exchanged(b_send, "tp", 6)
    a_next, b_next = quad_sums(keep, came, a1, b1, share)
    a2, b2 = exchanged(a_next, "tp", 6), exchanged(b_next, "tp", 2)
    leaving = leaving_rows(
        keep, came, a1, b1, a2, b2, weight, arrival, ep_count * slots, share
    )
    returned = lax.all_to_all(
        leaving.reshape(ep_count, slots, share), "ep", split_axis=0, concat_axis=0, tiled=True
    )
    merged, squares = merged_rows(group, stream, sel, returned.reshape(-1, share), share)
    totals = squares.reshape(1, tok_rows)
    for mask in (1, 2, 6):
        totals = totals + exchanged(totals, "tp", mask)
    scale_out = lax.rsqrt(totals.reshape(tok_rows, 1) / model_width + EPSILON)
    return (merged * scale_out * final_gain.astype(F32)[None, :]).astype(BF16)


def solution(mesh):
    return jax.shard_map(
        on_device,
        mesh=mesh,
        in_specs=(
            P("ep", None),
            P(),
            P(),
            P("ep", None),
            P("ep", None, "tp"),
            P("ep", None, "tp"),
            P("ep", "tp", None),
            P("tp"),
        ),
        out_specs=P("ep", "tp"),
        check_vma=False,
    )
```

```python
import functools

import jax
import jax.numpy as jnp
from jax import lax
from jax.experimental import pallas as pl
from jax.experimental.pallas import tpu as pltpu
from jax.sharding import PartitionSpec as P


EPSILON = 1e-06
FIRST_ROWS = 640
F32 = jnp.float32
BF16 = jnp.bfloat16


def exchanged(array, axis, mask):
    devices = lax.axis_size(axis)
    return lax.ppermute(array, axis, [(i, i ^ mask) for i in range(devices)])


def cost(flops, moved):
    return pl.CostEstimate(flops=int(flops), bytes_accessed=int(moved), transcendentals=0)


PARAMS = pltpu.CompilerParams(vmem_limit_bytes=28 * 1024 * 1024)


def shape_of(shape, dtype):
    return jax.ShapeDtypeStruct(shape, dtype)


def whole(shape):
    return pl.BlockSpec(shape, lambda *_: (0,) * len(shape))


def send_kernel(slots, where_ref, chosen_ref, stream_ref, gain_ref, out_ref, held, copied):
    load = pltpu.make_async_copy(stream_ref, held, copied)
    load.start()
    tokens, _ = held.shape
    share = out_ref.shape[1]
    column, base = where_ref[0], where_ref[1]
    chosen = chosen_ref[...]
    experts = chosen.shape[0]
    lane = lax.broadcasted_iota(jnp.int32, chosen.shape, 1)
    before = chosen < base
    inside = jnp.logical_not(before) & (chosen < base + tokens)
    begin = jnp.sum(jnp.where(before, 1.0, 0.0), axis=1, keepdims=True).astype(jnp.int32)
    slot = jnp.where(inside, lane - begin, -1)
    number = (chosen - base).astype(F32)
    lanes = gain_ref.shape[1]
    out_lane = lax.broadcasted_iota(jnp.int32, (experts, lanes), 1)
    picked = jnp.full((experts, lanes), -1.0, F32)
    for s in range(slots):
        hit = slot == s
        value = jnp.sum(jnp.where(hit, number + 1.0, 0.0), axis=1, keepdims=True) - 1.0
        picked = jnp.where(out_lane == s, value, picked)
    if experts < lanes:
        filler = jnp.full((lanes - experts, lanes), -1.0, F32)
        picked = jnp.concatenate([picked, filler], axis=0)
    by_slot = picked.T
    token = lax.broadcasted_iota(jnp.int32, (slots, tokens), 1).astype(F32)
    placed = jnp.concatenate(
        [
            jnp.where(token == by_slot[:slots, e : e + 1], 1.0, 0.0).astype(BF16)
            for e in range(experts)
        ],
        axis=0,
    )
    gains = gain_ref[...].astype(F32)
    groups = share // lanes
    gain_row = lax.broadcasted_iota(jnp.int32, gains.shape, 0)
    gain = jnp.concatenate(
        [
            jnp.sum(
                jnp.where(gain_row == column * groups + i, gains, 0.0), axis=0, keepdims=True
            )
            for i in range(groups)
        ],
        axis=1,
    )
    load.wait()
    x = held[...].astype(F32)
    scale = lax.rsqrt(jnp.mean(x * x, axis=-1, keepdims=True) + EPSILON)
    start = pl.multiple_of(column * share, lanes)
    own = (held[:, pl.ds(start, share)].astype(F32) * scale * gain).astype(BF16)
    out_ref[...] = jnp.dot(placed, own, preferred_element_type=F32).astype(BF16)


def outgoing_rows(where, chosen, stream, gain, slots, share):
    tokens, width = stream.shape
    experts = chosen.shape[0]
    return pl.pallas_call(
        functools.partial(send_kernel, slots),
        grid_spec=pltpu.PrefetchScalarGridSpec(
            num_scalar_prefetch=1,
            grid=(1,),
            in_specs=[
                whole(chosen.shape),
                pl.BlockSpec(memory_space=pltpu.MemorySpace.HBM),
                whole(gain.shape),
            ],
            out_specs=whole((experts * slots, share)),
            scratch_shapes=[pltpu.VMEM((tokens, width), BF16), pltpu.SemaphoreType.DMA],
        ),
        out_shape=shape_of((experts * slots, share), BF16),
        cost_estimate=cost(
            2 * experts * slots * tokens * share, 2 * tokens * width + 2 * experts * slots * share
        ),
        name="send_rows",
    )(where, chosen, stream, gain)


def compact_kernel(base, inv_ref, arrived_ref, out_ref):
    tile, slots = out_ref.shape[0], inv_ref.shape[1]
    at = lax.broadcasted_iota(jnp.int32, (tile, slots), 0) + (base + pl.program_id(0) * tile)
    hit = jnp.where(at == inv_ref[...], 1.0, 0.0).astype(BF16)
    out_ref[...] = jnp.dot(hit, arrived_ref[...], preferred_element_type=F32).astype(BF16)


def compacted(inv, arrived, base, picks):
    slots, width = arrived.shape
    tile = picks // 2
    return pl.pallas_call(
        functools.partial(compact_kernel, base),
        grid=(picks // tile,),
        in_specs=[whole((1, slots)), whole((slots, width))],
        out_specs=pl.BlockSpec((tile, width), lambda i: (i, 0)),
        out_shape=shape_of((picks, width), BF16),
        cost_estimate=cost(2 * picks * slots * width, 2 * slots * width),
        compiler_params=PARAMS,
        name="compact_rows",
    )(inv, arrived)


EARLY = (0, 1, 2, 3, 6, 7)


def products(pieces, gates, ups):
    total = None
    for piece, gate, up in zip(pieces, gates, ups):
        weights = jnp.concatenate([gate[...], up[...]], axis=1)
        part = jnp.dot(piece, weights, preferred_element_type=F32)
        total = part if total is None else total + part
    return total


def early_kernel(group_ref, *refs):
    n = len(EARLY)
    pieces = [ref[...] for ref in refs[:n]]
    refs[-1][...] = products(pieces, refs[n : 2 * n], refs[2 * n : 3 * n])


def late_kernel(group_ref, low, high, low_x, high_x, g4, g5, u4, u5, acc_ref, out_ref):
    upper = pl.program_id(0) >= pl.num_programs(0) // 2
    pieces = [
        jnp.where(upper, high[...], low[...]),
        jnp.where(upper, high_x[...], low_x[...]),
    ]
    total = acc_ref[...] + products(pieces, (g4, g5), (u4, u5))
    units = out_ref.shape[1]
    gate, up = total[:, :units], total[:, units:]
    out_ref[...] = (gate / (1.0 + jnp.exp(-gate)) * up).astype(BF16)


def weight_specs(masks, share, units):
    def spec(mask):
        return pl.BlockSpec((share, units), lambda i, g: (g[0] ^ mask, 0))

    return [spec(mask) for mask in masks]


def early_products(group, pieces, w_gate, w_up):
    picks, share = pieces[0].shape
    units = w_gate.shape[1]
    tile = picks // 2
    n = len(EARLY)
    return pl.pallas_call(
        early_kernel,
        grid_spec=pltpu.PrefetchScalarGridSpec(
            num_scalar_prefetch=1,
            grid=(picks // tile,),
            in_specs=[pl.BlockSpec((tile, share), lambda i, g: (i, 0))] * n
            + weight_specs(EARLY, share, units) * 2,
            out_specs=pl.BlockSpec((tile, 2 * units), lambda i, g: (i, 0)),
        ),
        out_shape=shape_of((picks, 2 * units), F32),
        cost_estimate=cost(4 * picks * n * share * units, 2 * n * share * (picks + 2 * units)),
        compiler_params=PARAMS,
        name="gate_up_early",
    )(group, *pieces, *([w_gate] * n), *([w_up] * n))


def late_products(group, halves, w_gate, w_up, acc):
    half, share = halves[0].shape
    picks = 2 * half
    units = w_gate.shape[1]
    tile = half
    steps = picks // tile
    low_spec = pl.BlockSpec((tile, share), lambda i, g: (jnp.minimum(i, steps // 2 - 1), 0))
    high_spec = pl.BlockSpec((tile, share), lambda i, g: (jnp.maximum(i - steps // 2, 0), 0))
    return pl.pallas_call(
        late_kernel,
        grid_spec=pltpu.PrefetchScalarGridSpec(
            num_scalar_prefetch=1,
            grid=(steps,),
            in_specs=[low_spec, high_spec] * 2
            + weight_specs((4, 5), share, units) * 2
            + [pl.BlockSpec((tile, 2 * units), lambda i, g: (i, 0))],
            out_specs=pl.BlockSpec((tile, units), lambda i, g: (i, 0)),
        ),
        out_shape=shape_of((picks, units), BF16),
        cost_estimate=cost(8 * picks * share * units, 4 * share * (picks + 2 * units)),
        compiler_params=PARAMS,
        name="gate_up_late",
    )(group, *halves, *([w_gate] * 2), *([w_up] * 2), acc)


def down_kernel(group_ref, hidden_ref, *refs):
    weights, out_ref = refs[:4], refs[4]
    side = jnp.concatenate([ref[...] for ref in weights], axis=1)
    out_ref[...] = jnp.dot(hidden_ref[...], side, preferred_element_type=F32).astype(BF16)


def down_products(group, hidden, w_down, core):
    picks, units = hidden.shape
    share = w_down.shape[1] // 8
    tile = picks // 2

    def spec(mask):
        return pl.BlockSpec((units, share), lambda i, g: (0, g[0] ^ mask))

    return pl.pallas_call(
        down_kernel,
        grid_spec=pltpu.PrefetchScalarGridSpec(
            num_scalar_prefetch=1,
            grid=(picks // tile,),
            in_specs=[pl.BlockSpec((tile, units), lambda i, g: (i, 0))]
            + [spec(2 * d + core) for d in range(4)],
            out_specs=pl.BlockSpec((tile, 4 * share), lambda i, g: (i, 0)),
        ),
        out_shape=shape_of((picks, 4 * share), BF16),
        cost_estimate=cost(8 * picks * share * units, 8 * (picks + units) * share),
        compiler_params=PARAMS,
        name="down",
    )(group, hidden, *([w_down] * 4))


def added(*refs):
    total = refs[0][...].astype(F32)
    for ref in refs[1:]:
        total = total + ref[...].astype(F32)
    return total


def pair_kernel(*refs):
    (a_ref, b_ref) = refs[8:]
    share = refs[0].shape[1]
    for out_ref, first in ((a_ref, 0), (b_ref, 4)):
        for n in range(2):
            out_ref[:, n * share : (n + 1) * share] = added(
                refs[first + 2 * n], refs[first + 2 * n + 1]
            ).astype(BF16)


def pair_sums(keep, came, share):
    picks = keep.shape[0]
    half = tile = picks // 2

    def spec(side, d):
        return pl.BlockSpec((tile, share), lambda i: (i + side * (half // tile), d))

    picked = [(0, 1), (0, 2), (1, 3), (1, 2)]
    specs = []
    for side, d in picked:
        specs += [spec(side, d)] * 2
    return pl.pallas_call(
        pair_kernel,
        grid=(half // tile,),
        in_specs=specs,
        out_specs=[pl.BlockSpec((tile, 2 * share), lambda i: (i, 0))] * 2,
        out_shape=[shape_of((half, 2 * share), BF16)] * 2,
        cost_estimate=cost(half * 4 * share, 24 * half * share),
        compiler_params=PARAMS,
        name="pair_sums",
    )(*([keep, came] * 4))


def quad_kernel(a0, a1, a2, b0, b1, b2, low0, low1, low2, high0, high1, high2, a_ref, b_ref, own_ref):
    a_ref[...] = added(a0, a1, a2).astype(BF16)
    b_ref[...] = added(b0, b1, b2).astype(BF16)
    half = a_ref.shape[0]
    own_ref[:half] = added(low0, low1, low2)
    own_ref[half:] = added(high0, high1, high2)


def quad_sums(keep, came, a_came, b_came, share):
    picks = keep.shape[0]
    half = picks // 2

    def spec(side, d):
        return pl.BlockSpec((half, share), lambda i: (side, d))

    first, second = spec(0, 0), spec(0, 1)
    out = spec(0, 0)
    return pl.pallas_call(
        quad_kernel,
        grid=(1,),
        in_specs=[spec(0, 3)] * 2
        + [second]
        + [spec(1, 1)] * 2
        + [second]
        + [spec(0, 0)] * 2
        + [first]
        + [spec(1, 0)] * 2
        + [first],
        out_specs=[out, out, whole((picks, share))],
        out_shape=[shape_of((half, share), BF16)] * 2 + [shape_of((picks, share), F32)],
        cost_estimate=cost(picks * 4 * share, 16 * picks * share),
        compiler_params=PARAMS,
        name="quad_sums",
    )(keep, came, a_came, keep, came, b_came, keep, came, a_came, keep, came, b_came)


def leave_kernel(own_ref, a2, b2, weight_ref, arrival_ref, *refs):
    out_ref, rows_ref = refs[-2:]
    half = a2.shape[0]

    @pl.when(pl.program_id(0) == 0)
    def _():
        weight = weight_ref[...]
        rows_ref[:half] = (added(own_ref.at[:half], a2) * weight[:half]).astype(BF16)
        rows_ref[half:] = (added(own_ref.at[half:], b2) * weight[half:]).astype(BF16)

    tile, picks = out_ref.shape[0], arrival_ref.shape[1]
    at = lax.broadcasted_iota(jnp.int32, (tile, picks), 0) + pl.program_id(0) * tile
    hit = jnp.where(at == arrival_ref[...], 1.0, 0.0).astype(BF16)
    total = jnp.dot(hit, rows_ref[...], preferred_element_type=F32)
    if len(refs) == 3:
        total = total + refs[0][...].astype(F32)
    out_ref[...] = total.astype(BF16)


def leaving_rows(own, a2, b2, weight, arrival, before, slots, share):
    picks = own.shape[0]
    half = picks // 2
    tile = slots // 3
    row_spec = pl.BlockSpec((tile, share), lambda i: (i, 0))
    return pl.pallas_call(
        leave_kernel,
        grid=(slots // tile,),
        in_specs=[whole((picks, share))]
        + [whole((half, share))] * 2
        + [
            whole((picks, 1)),
            whole((1, picks)),
        ]
        + [row_spec] * len(before),
        out_specs=row_spec,
        out_shape=shape_of((slots, share), BF16),
        scratch_shapes=[pltpu.VMEM((picks, share), BF16)],
        cost_estimate=cost(2 * slots * picks * share, 2 * (slots + 4 * picks) * share),
        compiler_params=PARAMS,
        name="leave_rows",
    )(own, a2, b2, weight, arrival, *before)


def merge_kernel(own_ref, sel_ref, came_ref, merged_ref, square_ref):
    tokens = own_ref.shape[0]
    sel = sel_ref[...]
    hit = lax.broadcasted_iota(jnp.int32, (tokens, sel.shape[1]), 0) == sel
    placed = jnp.where(hit, 1.0, 0.0).astype(BF16)
    update = jnp.dot(placed, came_ref[...], preferred_element_type=F32)
    merged = own_ref[...].astype(F32) + update
    merged_ref[...] = merged
    square_ref[...] = jnp.sum(merged * merged, axis=1, keepdims=True)


def merged_rows(own, sel, came):
    tokens, share = own.shape
    return pl.pallas_call(
        merge_kernel,
        out_shape=[shape_of((tokens, share), F32), shape_of((tokens, 1), F32)],
        cost_estimate=cost(2 * came.size * tokens, 2 * came.size),
        compiler_params=PARAMS,
        name="merge_rows",
    )(own, sel, came)


def on_device(stream, ffn_gain, chosen, affinity, w_gate, w_up, w_down, final_gain):
    tok_rows, model_width = stream.shape
    experts, picks = chosen.shape
    ep_count = lax.axis_size("ep")
    tp_count = lax.axis_size("tp")
    device = lax.axis_index("ep")
    column = lax.axis_index("tp").astype(jnp.int32)
    share = model_width // tp_count
    slots = 3 * tok_rows // 16
    group = column.reshape(1)

    base = device * tok_rows
    begin = jnp.sum((chosen < base).astype(jnp.int32), axis=1)
    end = jnp.sum((chosen < base + tok_rows).astype(jnp.int32), axis=1)
    slot_range = jnp.arange(slots, dtype=jnp.int32)
    places = jnp.arange(picks, dtype=jnp.int32)
    want = begin[:, None] + slot_range[None, :]
    found = jnp.sum(
        jnp.where(places[None, None, :] == want[:, :, None], chosen[:, None, :], 0), axis=2
    )
    sel = jnp.where(want < end[:, None], found - base, -1).reshape(1, experts * slots)

    row = lax.dynamic_index_in_dim(chosen, device, 0, keepdims=True)
    edges = jnp.arange(ep_count, dtype=jnp.int32)[:, None] * tok_rows
    starts = jnp.sum((row < edges).astype(jnp.int32), axis=1)
    stops = jnp.sum((row < edges + tok_rows).astype(jnp.int32), axis=1)
    row_want = starts[:, None] + slot_range[None, :]
    inv = jnp.where(row_want < stops[:, None], row_want, -1).reshape(1, ep_count * slots)
    mine = (row >= edges) & (row < edges + tok_rows)
    arrival = jnp.sum(
        jnp.where(
            mine,
            jnp.arange(ep_count, dtype=jnp.int32)[:, None] * slots
            + places[None, :]
            - starts[:, None],
            0,
        ),
        axis=0,
        keepdims=True,
    )
    weight = affinity.reshape(picks, 1)

    edges_of = (0, FIRST_ROWS, picks)
    parts = len(edges_of) - 1
    gate_rows, up_rows, down_rows = w_gate[0], w_up[0], w_down[0]
    own_stream = lax.dynamic_slice_in_dim(stream, column * share, share, 1)
    where = jnp.stack([column, base.astype(jnp.int32)])
    outgoing = outgoing_rows(where, chosen, stream, ffn_gain.reshape(-1, 128), slots, share)
    arrived = lax.all_to_all(
        outgoing.reshape(experts, slots, share), "ep", split_axis=0, concat_axis=0, tiled=True
    ).reshape(-1, share)

    def moved(array, mask):
        return exchanged(array, "tp", mask)

    keeps, cames, sends, leaving = [], [], [], []
    for part in range(parts):
        rows_from, rows_to = edges_of[part], edges_of[part + 1]
        half = (rows_to - rows_from) // 2
        own = compacted(inv, arrived, rows_from, rows_to - rows_from)
        near = moved(own, 2)
        back = moved(own, 6)
        far_low = moved(near[:half], 6)
        far_high = moved(back[half:], 2)
        pieces = [own, moved(own, 1), near, moved(near, 1), back, moved(back, 1)]
        halves = [far_low, far_high, moved(far_low, 1), moved(far_high, 1)]
        acc = early_products(group, pieces, gate_rows, up_rows)
        hidden = late_products(group, halves, gate_rows, up_rows, acc)
        give = down_products(group, hidden, down_rows, 1)
        keeps.append(down_products(group, hidden, down_rows, 0))
        cames.append(moved(give, 1))
        sends.append(pair_sums(keeps[part], cames[part], share))
    for part in range(parts):
        a1 = moved(sends[part][0], 2)
        b1 = moved(sends[part][1], 6)
        a_next, b_next, own_sum = quad_sums(keeps[part], cames[part], a1, b1, share)
        a2 = moved(a_next, 6)
        b2 = moved(b_next, 2)
        leaving = [
            leaving_rows(
                own_sum,
                a2,
                b2,
                weight[edges_of[part] : edges_of[part + 1]],
                arrival[:, edges_of[part] : edges_of[part + 1]],
                leaving,
                ep_count * slots,
                share,
            )
        ]
    returned = lax.all_to_all(
        leaving[0].reshape(ep_count, slots, share), "ep", split_axis=0, concat_axis=0, tiled=True
    )
    merged, squares = merged_rows(own_stream, sel, returned.reshape(-1, share))
    totals = squares.reshape(1, tok_rows)
    totals = totals + exchanged(totals, "tp", 1)
    totals = totals + sum(exchanged(totals, "tp", mask) for mask in (2, 4, 6))
    scale_out = lax.rsqrt(totals.reshape(tok_rows, 1) / model_width + EPSILON)
    return (merged * scale_out * final_gain.astype(F32)[None, :]).astype(BF16)


def solution(mesh):
    return jax.shard_map(
        on_device,
        mesh=mesh,
        in_specs=(
            P("ep", None),
            P(),
            P(),
            P("ep", None),
            P("ep", None, "tp"),
            P("ep", None, "tp"),
            P("ep", "tp", None),
            P("tp"),
        ),
        out_specs=P("ep", "tp"),
        check_vma=False,
    )
```

```python
import functools

import jax
import jax.numpy as jnp
from jax import lax
from jax.experimental import pallas as pl
from jax.experimental.pallas import tpu as pltpu
from jax.sharding import PartitionSpec as P


EPSILON = 1e-06
FIRST_ROWS = 576
F32 = jnp.float32
BF16 = jnp.bfloat16


def exchanged(array, axis, mask):
    devices = lax.axis_size(axis)
    return lax.ppermute(array, axis, [(i, i ^ mask) for i in range(devices)])


def cost(flops, moved):
    return pl.CostEstimate(flops=int(flops), bytes_accessed=int(moved), transcendentals=0)


PARAMS = pltpu.CompilerParams(vmem_limit_bytes=28 * 1024 * 1024)


def shape_of(shape, dtype):
    return jax.ShapeDtypeStruct(shape, dtype)


def whole(shape):
    return pl.BlockSpec(shape, lambda *_: (0,) * len(shape))


def send_kernel(slots, chosen_ref, stream_ref, gain_ref, out_ref, held, copied):
    load = pltpu.make_async_copy(stream_ref, held, copied)
    load.start()
    tokens, _ = held.shape
    share = out_ref.shape[1]
    column = lax.axis_index("tp").astype(jnp.int32)
    base = lax.axis_index("ep").astype(jnp.int32) * tokens
    chosen = chosen_ref[...]
    experts = chosen.shape[0]
    lane = lax.broadcasted_iota(jnp.int32, chosen.shape, 1)
    before = chosen < base
    inside = jnp.logical_not(before) & (chosen < base + tokens)
    begin = jnp.sum(jnp.where(before, 1.0, 0.0), axis=1, keepdims=True).astype(jnp.int32)
    slot = jnp.where(inside, lane - begin, -1)
    number = (chosen - base).astype(F32)
    lanes = gain_ref.shape[1]
    out_lane = lax.broadcasted_iota(jnp.int32, (experts, lanes), 1)
    picked = jnp.full((experts, lanes), -1.0, F32)
    for s in range(slots):
        hit = slot == s
        value = jnp.sum(jnp.where(hit, number + 1.0, 0.0), axis=1, keepdims=True) - 1.0
        picked = jnp.where(out_lane == s, value, picked)
    if experts < lanes:
        filler = jnp.full((lanes - experts, lanes), -1.0, F32)
        picked = jnp.concatenate([picked, filler], axis=0)
    by_slot = picked.T
    token = lax.broadcasted_iota(jnp.int32, (slots, tokens), 1).astype(F32)
    placed = jnp.concatenate(
        [
            jnp.where(token == by_slot[:slots, e : e + 1], 1.0, 0.0).astype(BF16)
            for e in range(experts)
        ],
        axis=0,
    )
    gains = gain_ref[...].astype(F32)
    groups = share // lanes
    gain_row = lax.broadcasted_iota(jnp.int32, gains.shape, 0)
    gain = jnp.concatenate(
        [
            jnp.sum(
                jnp.where(gain_row == column * groups + i, gains, 0.0), axis=0, keepdims=True
            )
            for i in range(groups)
        ],
        axis=1,
    )
    load.wait()
    x = held[...].astype(F32)
    scale = lax.rsqrt(jnp.mean(x * x, axis=-1, keepdims=True) + EPSILON)
    start = pl.multiple_of(column * share, lanes)
    own = (held[:, pl.ds(start, share)].astype(F32) * scale * gain).astype(BF16)
    out_ref[...] = jnp.dot(placed, own, preferred_element_type=F32).astype(BF16)


def outgoing_rows(chosen, stream, gain, slots, share):
    tokens, width = stream.shape
    experts = chosen.shape[0]
    return pl.pallas_call(
        functools.partial(send_kernel, slots),
        grid=(1,),
        in_specs=[
            whole(chosen.shape),
            pl.BlockSpec(memory_space=pltpu.MemorySpace.HBM),
            whole(gain.shape),
        ],
        out_specs=whole((experts * slots, share)),
        scratch_shapes=[pltpu.VMEM((tokens, width), BF16), pltpu.SemaphoreType.DMA],
        out_shape=shape_of((experts * slots, share), BF16),
        cost_estimate=cost(
            2 * experts * slots * tokens * share, 2 * tokens * width + 2 * experts * slots * share
        ),
        name="send_rows",
    )(chosen, stream, gain)


def compact_kernel(base, inv_ref, arrived_ref, out_ref):
    tile, slots = out_ref.shape[0], inv_ref.shape[1]
    at = lax.broadcasted_iota(jnp.int32, (tile, slots), 0) + (base + pl.program_id(0) * tile)
    hit = jnp.where(at == inv_ref[...], 1.0, 0.0).astype(BF16)
    out_ref[...] = jnp.dot(hit, arrived_ref[...], preferred_element_type=F32).astype(BF16)


def compacted(inv, arrived, base, picks):
    slots, width = arrived.shape
    tile = picks // 2
    return pl.pallas_call(
        functools.partial(compact_kernel, base),
        grid=(picks // tile,),
        in_specs=[whole((1, slots)), whole((slots, width))],
        out_specs=pl.BlockSpec((tile, width), lambda i: (i, 0)),
        out_shape=shape_of((picks, width), BF16),
        cost_estimate=cost(2 * picks * slots * width, 2 * slots * width),
        compiler_params=PARAMS,
        name="compact_rows",
    )(inv, arrived)


def cut_kernel(near_ref, back_ref, low_ref, high_ref):
    half = low_ref.shape[0]
    low_ref[...] = near_ref[:half]
    high_ref[...] = back_ref[half:]


def halves_of(near, back):
    rows, share = near.shape
    half = shape_of((rows // 2, share), near.dtype)
    return pl.pallas_call(
        cut_kernel,
        out_shape=[half, half],
        cost_estimate=cost(0, 4 * rows * share),
        compiler_params=PARAMS,
        name="halves",
    )(near, back)


EARLY = (0, 1, 2, 3, 6, 7)


def products(pieces, gates, ups):
    total = None
    for piece, gate, up in zip(pieces, gates, ups):
        weights = jnp.concatenate([gate[...], up[...]], axis=1)
        part = jnp.dot(piece, weights, preferred_element_type=F32)
        total = part if total is None else total + part
    return total


def early_kernel(group_ref, *refs):
    n = len(EARLY)
    pieces = [ref[...] for ref in refs[:n]]
    refs[-1][...] = products(pieces, refs[n : 2 * n], refs[2 * n : 3 * n])


def late_kernel(group_ref, low, high, low_x, high_x, g4, g5, u4, u5, acc_ref, out_ref):
    upper = pl.program_id(0) >= pl.num_programs(0) // 2
    pieces = [
        jnp.where(upper, high[...], low[...]),
        jnp.where(upper, high_x[...], low_x[...]),
    ]
    total = acc_ref[...] + products(pieces, (g4, g5), (u4, u5))
    units = out_ref.shape[1]
    gate, up = total[:, :units], total[:, units:]
    out_ref[...] = (gate / (1.0 + jnp.exp(-gate)) * up).astype(BF16)


def weight_specs(masks, share, units):
    def spec(mask):
        return pl.BlockSpec((share, units), lambda i, g: (g[0] ^ mask, 0))

    return [spec(mask) for mask in masks]


def early_products(group, pieces, w_gate, w_up):
    picks, share = pieces[0].shape
    units = w_gate.shape[1]
    tile = picks
    n = len(EARLY)
    return pl.pallas_call(
        early_kernel,
        grid_spec=pltpu.PrefetchScalarGridSpec(
            num_scalar_prefetch=1,
            grid=(picks // tile,),
            in_specs=[pl.BlockSpec((tile, share), lambda i, g: (i, 0))] * n
            + weight_specs(EARLY, share, units) * 2,
            out_specs=pl.BlockSpec((tile, 2 * units), lambda i, g: (i, 0)),
        ),
        out_shape=shape_of((picks, 2 * units), F32),
        cost_estimate=cost(4 * picks * n * share * units, 2 * n * share * (picks + 2 * units)),
        compiler_params=PARAMS,
        name="gate_up_early",
    )(group, *pieces, *([w_gate] * n), *([w_up] * n))


def late_products(group, halves, w_gate, w_up, acc):
    half, share = halves[0].shape
    picks = 2 * half
    units = w_gate.shape[1]
    tile = half
    steps = picks // tile
    low_spec = pl.BlockSpec((tile, share), lambda i, g: (jnp.minimum(i, steps // 2 - 1), 0))
    high_spec = pl.BlockSpec((tile, share), lambda i, g: (jnp.maximum(i - steps // 2, 0), 0))
    return pl.pallas_call(
        late_kernel,
        grid_spec=pltpu.PrefetchScalarGridSpec(
            num_scalar_prefetch=1,
            grid=(steps,),
            in_specs=[low_spec, high_spec] * 2
            + weight_specs((4, 5), share, units) * 2
            + [pl.BlockSpec((tile, 2 * units), lambda i, g: (i, 0))],
            out_specs=pl.BlockSpec((tile, units), lambda i, g: (i, 0)),
        ),
        out_shape=shape_of((picks, units), BF16),
        cost_estimate=cost(8 * picks * share * units, 4 * share * (picks + 2 * units)),
        compiler_params=PARAMS,
        name="gate_up_late",
    )(group, *halves, *([w_gate] * 2), *([w_up] * 2), acc)


def down_kernel(group_ref, hidden_ref, *refs):
    weights, out_ref = refs[:4], refs[4]
    side = jnp.concatenate([ref[...] for ref in weights], axis=1)
    out_ref[...] = jnp.dot(hidden_ref[...], side, preferred_element_type=F32).astype(BF16)


def down_products(group, hidden, w_down, core):
    picks, units = hidden.shape
    share = w_down.shape[1] // 8
    tile = picks

    def spec(mask):
        return pl.BlockSpec((units, share), lambda i, g: (0, g[0] ^ mask))

    return pl.pallas_call(
        down_kernel,
        grid_spec=pltpu.PrefetchScalarGridSpec(
            num_scalar_prefetch=1,
            grid=(picks // tile,),
            in_specs=[pl.BlockSpec((tile, units), lambda i, g: (i, 0))]
            + [spec(2 * d + core) for d in range(4)],
            out_specs=pl.BlockSpec((tile, 4 * share), lambda i, g: (i, 0)),
        ),
        out_shape=shape_of((picks, 4 * share), BF16),
        cost_estimate=cost(8 * picks * share * units, 8 * (picks + units) * share),
        compiler_params=PARAMS,
        name="down",
    )(group, hidden, *([w_down] * 4))


def added(*refs):
    total = refs[0][...].astype(F32)
    for ref in refs[1:]:
        total = total + ref[...].astype(F32)
    return total


def pair_kernel(*refs):
    (a_ref, b_ref) = refs[8:]
    share = refs[0].shape[1]
    for out_ref, first in ((a_ref, 0), (b_ref, 4)):
        for n in range(2):
            out_ref[:, n * share : (n + 1) * share] = added(
                refs[first + 2 * n], refs[first + 2 * n + 1]
            ).astype(BF16)


def pair_sums(keep, came, share):
    picks = keep.shape[0]
    half = tile = picks // 2

    def spec(side, d):
        return pl.BlockSpec((tile, share), lambda i: (i + side * (half // tile), d))

    picked = [(0, 1), (0, 2), (1, 3), (1, 2)]
    specs = []
    for side, d in picked:
        specs += [spec(side, d)] * 2
    return pl.pallas_call(
        pair_kernel,
        grid=(half // tile,),
        in_specs=specs,
        out_specs=[pl.BlockSpec((tile, 2 * share), lambda i: (i, 0))] * 2,
        out_shape=[shape_of((half, 2 * share), BF16)] * 2,
        cost_estimate=cost(half * 4 * share, 24 * half * share),
        compiler_params=PARAMS,
        name="pair_sums",
    )(*([keep, came] * 4))


def quad_kernel(a0, a1, a2, b0, b1, b2, low0, low1, low2, high0, high1, high2, a_ref, b_ref, own_ref):
    a_ref[...] = added(a0, a1, a2).astype(BF16)
    b_ref[...] = added(b0, b1, b2).astype(BF16)
    half = a_ref.shape[0]
    own_ref[:half] = added(low0, low1, low2)
    own_ref[half:] = added(high0, high1, high2)


def quad_sums(keep, came, a_came, b_came, share):
    picks = keep.shape[0]
    half = picks // 2

    def spec(side, d):
        return pl.BlockSpec((half, share), lambda i: (side, d))

    first, second = spec(0, 0), spec(0, 1)
    out = spec(0, 0)
    return pl.pallas_call(
        quad_kernel,
        grid=(1,),
        in_specs=[spec(0, 3)] * 2
        + [second]
        + [spec(1, 1)] * 2
        + [second]
        + [spec(0, 0)] * 2
        + [first]
        + [spec(1, 0)] * 2
        + [first],
        out_specs=[out, out, whole((picks, share))],
        out_shape=[shape_of((half, share), BF16)] * 2 + [shape_of((picks, share), F32)],
        cost_estimate=cost(picks * 4 * share, 16 * picks * share),
        compiler_params=PARAMS,
        name="quad_sums",
    )(keep, came, a_came, keep, came, b_came, keep, came, a_came, keep, came, b_came)


def leave_kernel(own_ref, a2, b2, weight_ref, arrival_ref, *refs):
    out_ref, rows_ref = refs[-2:]
    half = a2.shape[0]

    @pl.when(pl.program_id(0) == 0)
    def _():
        weight = weight_ref[...]
        rows_ref[:half] = (added(own_ref.at[:half], a2) * weight[:half]).astype(BF16)
        rows_ref[half:] = (added(own_ref.at[half:], b2) * weight[half:]).astype(BF16)

    tile, picks = out_ref.shape[0], arrival_ref.shape[1]
    at = lax.broadcasted_iota(jnp.int32, (tile, picks), 0) + pl.program_id(0) * tile
    hit = jnp.where(at == arrival_ref[...], 1.0, 0.0).astype(BF16)
    total = jnp.dot(hit, rows_ref[...], preferred_element_type=F32)
    if len(refs) == 3:
        total = total + refs[0][...].astype(F32)
    out_ref[...] = total.astype(BF16)


def leaving_rows(own, a2, b2, weight, arrival, before, slots, share):
    picks = own.shape[0]
    half = picks // 2
    tile = slots // 3
    row_spec = pl.BlockSpec((tile, share), lambda i: (i, 0))
    return pl.pallas_call(
        leave_kernel,
        grid=(slots // tile,),
        in_specs=[whole((picks, share))]
        + [whole((half, share))] * 2
        + [
            whole((picks, 1)),
            whole((1, picks)),
        ]
        + [row_spec] * len(before),
        out_specs=row_spec,
        out_shape=shape_of((slots, share), BF16),
        scratch_shapes=[pltpu.VMEM((picks, share), BF16)],
        cost_estimate=cost(2 * slots * picks * share, 2 * (slots + 4 * picks) * share),
        compiler_params=PARAMS,
        name="leave_rows",
    )(own, a2, b2, weight, arrival, *before)


def merge_kernel(own_ref, sel_ref, came_ref, merged_ref, square_ref):
    tokens = own_ref.shape[0]
    sel = sel_ref[...]
    hit = lax.broadcasted_iota(jnp.int32, (tokens, sel.shape[1]), 0) == sel
    placed = jnp.where(hit, 1.0, 0.0).astype(BF16)
    update = jnp.dot(placed, came_ref[...], preferred_element_type=F32)
    merged = own_ref[...].astype(F32) + update
    merged_ref[...] = merged
    square_ref[...] = jnp.sum(merged * merged, axis=1, keepdims=True)


def merged_rows(own, sel, came):
    tokens, share = own.shape
    return pl.pallas_call(
        merge_kernel,
        out_shape=[shape_of((tokens, share), F32), shape_of((tokens, 1), F32)],
        cost_estimate=cost(2 * came.size * tokens, 2 * came.size),
        compiler_params=PARAMS,
        name="merge_rows",
    )(own, sel, came)


def on_device(stream, ffn_gain, chosen, affinity, w_gate, w_up, w_down, final_gain):
    tok_rows, model_width = stream.shape
    experts, picks = chosen.shape
    ep_count = lax.axis_size("ep")
    tp_count = lax.axis_size("tp")
    device = lax.axis_index("ep")
    column = lax.axis_index("tp").astype(jnp.int32)
    share = model_width // tp_count
    slots = 3 * tok_rows // 16
    group = column.reshape(1)

    base = device * tok_rows
    begin = jnp.sum((chosen < base).astype(jnp.int32), axis=1)
    end = jnp.sum((chosen < base + tok_rows).astype(jnp.int32), axis=1)
    slot_range = jnp.arange(slots, dtype=jnp.int32)
    places = jnp.arange(picks, dtype=jnp.int32)
    want = begin[:, None] + slot_range[None, :]
    found = jnp.sum(
        jnp.where(places[None, None, :] == want[:, :, None], chosen[:, None, :], 0), axis=2
    )
    sel = jnp.where(want < end[:, None], found - base, -1).reshape(1, experts * slots)

    row = lax.dynamic_index_in_dim(chosen, device, 0, keepdims=True)
    edges = jnp.arange(ep_count, dtype=jnp.int32)[:, None] * tok_rows
    starts = jnp.sum((row < edges).astype(jnp.int32), axis=1)
    stops = jnp.sum((row < edges + tok_rows).astype(jnp.int32), axis=1)
    row_want = starts[:, None] + slot_range[None, :]
    inv = jnp.where(row_want < stops[:, None], row_want, -1).reshape(1, ep_count * slots)
    mine = (row >= edges) & (row < edges + tok_rows)
    arrival = jnp.sum(
        jnp.where(
            mine,
            jnp.arange(ep_count, dtype=jnp.int32)[:, None] * slots
            + places[None, :]
            - starts[:, None],
            0,
        ),
        axis=0,
        keepdims=True,
    )

    edges_of = (0, FIRST_ROWS, picks)
    spans = list(zip(edges_of, edges_of[1:]))
    weights = [affinity[0, low:high].reshape(-1, 1) for low, high in spans]
    arrivals = [arrival[:, low:high] for low, high in spans]
    parts = len(edges_of) - 1
    gate_rows, up_rows, down_rows = w_gate[0], w_up[0], w_down[0]
    own_stream = lax.dynamic_slice_in_dim(stream, column * share, share, 1)
    outgoing = outgoing_rows(chosen, stream, ffn_gain.reshape(-1, 128), slots, share)
    arrived = lax.all_to_all(
        outgoing.reshape(experts, slots, share), "ep", split_axis=0, concat_axis=0, tiled=True
    ).reshape(-1, share)

    arrived, sel, inv, arrivals, weights, own_stream = lax.optimization_barrier(
        (arrived, sel, inv, arrivals, weights, own_stream)
    )

    def moved(array, mask):
        return exchanged(array, "tp", mask)

    keeps, cames, sends, leaving = [], [], [], []
    for part in range(parts):
        rows_from, rows_to = edges_of[part], edges_of[part + 1]
        own = compacted(inv, arrived, rows_from, rows_to - rows_from)
        near = moved(own, 2)
        back = moved(own, 6)
        low, high = halves_of(near, back)
        far_low = moved(low, 6)
        far_high = moved(high, 2)
        pieces = [own, moved(own, 1), near, moved(near, 1), back, moved(back, 1)]
        halves = [far_low, far_high, moved(far_low, 1), moved(far_high, 1)]
        acc = early_products(group, pieces, gate_rows, up_rows)
        hidden = late_products(group, halves, gate_rows, up_rows, acc)
        give = down_products(group, hidden, down_rows, 1)
        keeps.append(down_products(group, hidden, down_rows, 0))
        cames.append(moved(give, 1))
        sends.append(pair_sums(keeps[part], cames[part], share))
    for part in range(parts):
        a1 = moved(sends[part][0], 2)
        b1 = moved(sends[part][1], 6)
        a_next, b_next, own_sum = quad_sums(keeps[part], cames[part], a1, b1, share)
        a2 = moved(a_next, 6)
        b2 = moved(b_next, 2)
        leaving = [
            leaving_rows(
                own_sum, a2, b2, weights[part], arrivals[part], leaving, ep_count * slots, share
            )
        ]
    returned = lax.all_to_all(
        leaving[0].reshape(ep_count, slots, share), "ep", split_axis=0, concat_axis=0, tiled=True
    )
    merged, squares = merged_rows(own_stream, sel, returned.reshape(-1, share))
    totals = squares.reshape(1, tok_rows)
    totals = totals + exchanged(totals, "tp", 1)
    totals = totals + sum(exchanged(totals, "tp", mask) for mask in (2, 4, 6))
    scale_out = lax.rsqrt(totals.reshape(tok_rows, 1) / model_width + EPSILON)
    return (merged * scale_out * final_gain.astype(F32)[None, :]).astype(BF16)


def solution(mesh):
    return jax.shard_map(
        on_device,
        mesh=mesh,
        in_specs=(
            P("ep", None),
            P(),
            P(),
            P("ep", None),
            P("ep", None, "tp"),
            P("ep", None, "tp"),
            P("ep", "tp", None),
            P("tp"),
        ),
        out_specs=P("ep", "tp"),
        check_vma=False,
    )
```
